32 devices in a mesh: sp: 4 (over z), tp: 4 (over y, x), dp: 2 (over core).
Axes of the slice: x: 2, y: 2, z: 4, core: 2. Of those that a mesh axis runs over, the one named last changes fastest.
Arguments:
- latent_in: bfloat16 [3072, 2048], P(('dp', 'sp', 'tp')), parts along dimension 0, may hold values from -6 to 6
- condition: bfloat16 [4096], P(('dp', 'sp')), parts along dimension 0, may hold values from -8 to 8
- context_latent: bfloat16 [1024, 256], P(('dp', 'sp')), parts along dimension 0, may hold values from -6 to 6
- context_rope: bfloat16 [1024, 64], P(('dp', 'sp')), parts along dimension 0, may hold values from -6 to 6
- shift_weight: bfloat16 [2048, 2048], P('sp', 'tp'), may hold values from -0.125 to 0.125
- scale_weight: bfloat16 [2048, 2048], P('sp', 'tp'), may hold values from -0.125 to 0.125
- gate_weight: bfloat16 [2048, 2048], P('sp', 'tp'), may hold values from -0.125 to 0.125
- norm_gain: float32 [2048], replicated, may hold values from 0.1 to 1.9
- down_query: bfloat16 [2048, 512], replicated, may hold values from -0.125 to 0.125
- down_latent: bfloat16 [2048, 256], replicated, may hold values from -0.125 to 0.125
- down_rope: bfloat16 [2048, 64], replicated, may hold values from -0.125 to 0.125
- query_gain: float32 [512], replicated, may hold values from 0.5 to 60
- latent_gain: float32 [256], replicated, may hold values from 0.1 to 1.9
- up_query: bfloat16 [512, 1536], P(None, 'tp'), may hold values from -0.25 to 0.25
- up_key: bfloat16 [256, 1024], P(None, 'tp'), may hold values from -0.375 to 0.375
- up_value: bfloat16 [256, 1024], P(None, 'tp'), may hold values from -0.375 to 0.375
- context_bias: float32 [8], P('tp'), may hold values from 1 to 2.5
- out_weight: bfloat16 [1024, 2048], replicated, may hold values from -3 to 3
Outputs:
- mixed_out: bfloat16 [3072, 2048], P(('dp', 'sp', 'tp')), parts along dimension 0
The draws below stay inside these ranges and needn't reach their ends.
There are 2 independent parts, one for each index of `dp`. The reference program is written for one: setup_inputs(seed, part) draws one part's arguments, and reference() takes and returns one part's arrays. A program takes and returns all parts, laid end to end along the dimension named above; an argument that names none is the same for every part. Nothing has to cross between parts.
All inputs are finite; a program needn't handle non-finite values.
Results may differ from the reference program's by a relative error of at most 0.039.
The reference program's roundings to bfloat16 on the way count: a program that leaves them out, or rounds other values in their place, can miss the bound.
Values may be sent and summed in bfloat16 or wider, within the bound.
No kernel may reach another device: no remote copies, remote signals or barrier semaphores. Data moves between devices by JAX's collectives and lax.ppermute only.
A program may use at most 128 MiB of HBM per device.

```python
import math
import jax
import jax.numpy as jnp
from jax import lax

D = 2048
HEADS = 8
QK_NOPE = 128
QK_ROPE = 64
V_HEAD = 128
Q_RANK = 512
KV_RANK = 256
GRID_W = 64
CTX = 512
TOKENS = 1536


def draw_query_gain(key, part):
    gains = jax.random.uniform(key, (Q_RANK,), jnp.float32, 0.5, 1.5)
    return gains


def levels(rng, shape, cuts, low, high):
    def one(axis_at, blocks):
        draws = jax.random.uniform(jax.random.fold_in(jax.random.fold_in(rng, 6), axis_at), (blocks,), jnp.float32, low / len(cuts), high / len(cuts))
        return jnp.repeat(jnp.exp(draws), shape[axis_at] // blocks).reshape((-1,) + (1,) * (len(shape) - axis_at - 1))

    gain = one(*cuts[0])
    for cut in cuts[1:]:
        gain = gain * one(*cut)
    return gain


def noise(own_key, extent, scale, reach, cuts=(), kind=jnp.bfloat16):
    level = levels(own_key, extent, cuts, -0.22, 0.18) if cuts else 1.0
    entries = jax.random.normal(own_key, extent, jnp.float32) * scale * level
    return jnp.minimum(jnp.maximum(entries, -reach), reach).astype(kind)


def setup_inputs(seed: int = 0, part: int = 0) -> dict:
    splits = jax.random.split(jax.random.key(seed), 19)
    part_splits = jax.random.split(jax.random.fold_in(splits[18], part), 19)
    latent_in = noise(part_splits[0], (TOKENS, D), 1.0, 6.0, ((0, 16),))
    condition = noise(part_splits[1], (D,), 2.0, 8.0, ((0, 4),))
    context_latent = noise(part_splits[2], (CTX, KV_RANK), 1.0, 6.0, ((0, 4),))
    context_rope = noise(part_splits[3], (CTX, QK_ROPE), 1.0, 6.0, ((0, 4),))
    shift_weight = noise(splits[4], (D, D), D ** -0.5, 0.125, ((0, 4), (1, 4)))
    scale_weight = noise(splits[5], (D, D), D ** -0.5, 0.125, ((0, 4), (1, 4)))
    gate_weight = noise(splits[6], (D, D), D ** -0.5, 0.125, ((0, 4), (1, 4)))
    norm_gain = jnp.clip(1.0 + 0.18 * jax.random.normal(splits[7], (D,), jnp.float32), 0.1, 1.9)
    down_query = noise(splits[8], (D, Q_RANK), D ** -0.5, 0.125)
    down_latent = noise(splits[9], (D, KV_RANK), D ** -0.5, 0.125)
    down_rope = noise(splits[10], (D, QK_ROPE), D ** -0.5, 0.125)
    query_gain = draw_query_gain(jax.random.fold_in(splits[18], 71), part)
    latent_gain = jnp.clip(1.0 + 0.18 * jax.random.normal(splits[12], (KV_RANK,), jnp.float32), 0.1, 1.9)
    up_query = noise(splits[13], (Q_RANK, HEADS * (QK_NOPE + QK_ROPE)), Q_RANK ** -0.5, 0.25, ((1, 4),))
    up_key = noise(splits[14], (KV_RANK, HEADS * QK_NOPE), KV_RANK ** -0.5, 0.375, ((1, 4),))
    up_value = noise(splits[15], (KV_RANK, HEADS * V_HEAD), KV_RANK ** -0.5, 0.375, ((1, 4),))
    context_bias = jnp.clip(1.0 + 1.5 * jax.random.uniform(splits[16], (HEADS,), jnp.float32) ** levels(splits[16], (HEADS,), ((0, 4),), -0.2, 0.2), 1.0, 2.5)
    out_weight = noise(splits[17], (HEADS * V_HEAD, D), 0.5, 3.0)
    return dict(latent_in=latent_in, condition=condition, context_latent=context_latent, context_rope=context_rope, shift_weight=shift_weight, scale_weight=scale_weight, gate_weight=gate_weight, norm_gain=norm_gain, down_query=down_query, down_latent=down_latent, down_rope=down_rope, query_gain=query_gain, latent_gain=latent_gain, up_query=up_query, up_key=up_key, up_value=up_value, context_bias=context_bias, out_weight=out_weight)


epsilon = 1e-06
rope_base = 10000.0

def rms_scaled(values, gain_vec):
    mean_sq = lax.optimization_barrier(jnp.mean(values * values, axis=-1, keepdims=True))
    return values * lax.rsqrt(mean_sq + epsilon) * gain_vec

def rope_tables(positions, rope_width):
    freq_count = rope_width // 4
    inverse = rope_base ** (-jnp.arange(freq_count, dtype=jnp.float32) / freq_count)
    grid_row = (positions // GRID_W).astype(jnp.float32)
    grid_col = (positions % GRID_W).astype(jnp.float32)
    row_angle = grid_row[:, None] * inverse
    col_angle = grid_col[:, None] * inverse
    angles = jnp.concatenate([row_angle, row_angle, col_angle, col_angle], axis=-1)
    return (jnp.cos(angles), jnp.sin(angles))

def rope_turn(values, cosine_table, sine_table):
    part_one, part_two, part_three, part_four = jnp.split(values, 4, axis=-1)
    turned = jnp.concatenate([-part_two, part_one, -part_four, part_three], axis=-1)
    return values * cosine_table + turned * sine_table

def reference(latent_in, condition, context_latent, context_rope, shift_weight, scale_weight, gate_weight, norm_gain, down_query, down_latent, down_rope, query_gain, latent_gain, up_query, up_key, up_value, context_bias, out_weight):
    activated = jax.nn.silu(condition.astype(jnp.float32)).astype(jnp.bfloat16)
    shift_vec = jnp.dot(activated, shift_weight, preferred_element_type=jnp.float32)
    scale_vec = jnp.dot(activated, scale_weight, preferred_element_type=jnp.float32)
    gate_vec = jnp.dot(activated, gate_weight, preferred_element_type=jnp.float32)
    residual_in = latent_in.astype(jnp.float32)
    normed = (rms_scaled(residual_in, norm_gain) * (1.0 + scale_vec) + shift_vec).astype(jnp.bfloat16)
    query_low = rms_scaled(jnp.dot(normed, down_query, preferred_element_type=jnp.float32), query_gain).astype(jnp.bfloat16)
    latent_low = rms_scaled(jnp.dot(normed, down_latent, preferred_element_type=jnp.float32), latent_gain).astype(jnp.bfloat16)
    positions = jnp.arange(TOKENS, dtype=jnp.int32)
    cosine_table, sine_table = rope_tables(positions, QK_ROPE)
    rope_keys = rope_turn(jnp.dot(normed, down_rope, preferred_element_type=jnp.float32), cosine_table, sine_table).astype(jnp.bfloat16)
    queries = jnp.dot(query_low, up_query, preferred_element_type=jnp.float32).reshape(TOKENS, HEADS, QK_NOPE + QK_ROPE)
    query_rope = rope_turn(queries[:, :, QK_NOPE:], cosine_table[:, None, :], sine_table[:, None, :])
    queries = jnp.concatenate([queries[:, :, :QK_NOPE], query_rope], axis=-1).astype(jnp.bfloat16)
    all_latent = jnp.concatenate([context_latent, latent_low], axis=0)
    all_rope = jnp.concatenate([context_rope, rope_keys], axis=0)
    key_count = CTX + TOKENS
    keys_nope = jnp.dot(all_latent, up_key, preferred_element_type=jnp.float32).astype(jnp.bfloat16).reshape(key_count, HEADS, QK_NOPE)
    values_all = jnp.dot(all_latent, up_value, preferred_element_type=jnp.float32).astype(jnp.bfloat16).reshape(key_count, HEADS, V_HEAD)
    bias_row = jnp.concatenate([jnp.broadcast_to(context_bias[:, None], (HEADS, CTX)), jnp.zeros((HEADS, TOKENS), jnp.float32)], axis=1)[:, None, :]
    keys_wide = keys_nope.astype(jnp.float32)
    rope_wide = all_rope.astype(jnp.float32)
    values_wide = values_all.astype(jnp.float32)
    block_rows = math.gcd(TOKENS, 512)
    query_blocks = queries.astype(jnp.float32).reshape(TOKENS // block_rows, block_rows, HEADS, QK_NOPE + QK_ROPE)
    score_scale = (QK_NOPE + QK_ROPE) ** (-0.5)

    def one_block(query_block):
        scores = jnp.einsum('thd,khd->htk', query_block[:, :, :QK_NOPE], keys_wide)
        scores = scores + jnp.einsum('thr,kr->htk', query_block[:, :, QK_NOPE:], rope_wide)
        scores = scores * score_scale + bias_row
        row_max = lax.optimization_barrier(jnp.max(scores, axis=-1, keepdims=True))
        weights = jnp.exp(scores - row_max)
        totals = lax.optimization_barrier(jnp.sum(weights, axis=-1))
        rounded = lax.optimization_barrier(weights.astype(jnp.bfloat16)).astype(jnp.float32)
        summed = jnp.einsum('htk,khd->htd', rounded, values_wide)
        return (summed / totals[:, :, None]).astype(jnp.bfloat16)
    outputs = lax.map(one_block, query_blocks)
    attended = outputs.transpose(0, 2, 1, 3).reshape(TOKENS, HEADS * V_HEAD)
    mixed = jnp.dot(attended, out_weight, preferred_element_type=jnp.float32)
    return (residual_in + gate_vec * mixed).astype(jnp.bfloat16)
```

```python
import jax
import jax.numpy as jnp
from jax import lax
from jax.sharding import PartitionSpec as P

QK_NOPE = 128
QK_ROPE = 64
V_HEAD = 128
GRID_W = 64


epsilon = 1e-06
rope_base = 10000.0
block_limit = 2048


def rms_scaled(values, gain_vec):
    mean_sq = jnp.mean(values * values, axis=-1, keepdims=True)
    return values * lax.rsqrt(mean_sq + epsilon) * gain_vec


def rope_tables(positions, rope_width):
    freq_count = rope_width // 4
    inverse = rope_base ** (-jnp.arange(freq_count, dtype=jnp.float32) / freq_count)
    grid_row = (positions // GRID_W).astype(jnp.float32)
    grid_col = (positions % GRID_W).astype(jnp.float32)
    row_angle = grid_row[:, None] * inverse
    col_angle = grid_col[:, None] * inverse
    angles = jnp.concatenate([row_angle, row_angle, col_angle, col_angle], axis=-1)
    return (jnp.cos(angles), jnp.sin(angles))


def rope_turn(values, cosine_table, sine_table):
    part_one, part_two, part_three, part_four = jnp.split(values, 4, axis=-1)
    turned = jnp.concatenate([-part_two, part_one, -part_four, part_three], axis=-1)
    return values * cosine_table + turned * sine_table


def turn_columns(weights, rope_width):
    part_one, part_two, part_three, part_four = jnp.split(weights, 4, axis=-1)
    return jnp.concatenate([-part_two, part_one, -part_four, part_three], axis=-1)


def exchange_steps(axis):
    size = lax.axis_size(axis)
    steps = list(range(1, size))
    if size & (size - 1):
        return [
            (lambda at, s=s: (at + size - s) % size, [(i, (i + s) % size) for i in range(size)],
             lambda at, s=s: (at + s) % size)
            for s in steps
        ]
    return [(lambda at, s=s: at ^ s, [(i, i ^ s) for i in range(size)], lambda at, s=s: at ^ s) for s in steps]


def gather_pieces(piece, axis):
    return [lax.ppermute(piece, axis, pairs) for _, pairs, _ in exchange_steps(axis)]


def attend(query, keys_latent, keys_rope, up_key, up_value, bias_rows):
    head_count = query.shape[1]
    key_count = keys_latent.shape[0]
    score_scale = query.shape[-1] ** (-0.5)
    keys_nope = (
        jnp.dot(keys_latent, up_key, preferred_element_type=jnp.float32)
        .astype(jnp.bfloat16)
        .reshape(key_count, head_count, QK_NOPE)
    )
    values = (
        jnp.dot(keys_latent, up_value, preferred_element_type=jnp.float32)
        .astype(jnp.bfloat16)
        .reshape(key_count, head_count, V_HEAD)
    )
    accs, maxima, totals = [], [], []
    for head in range(head_count):
        scores = lax.dot_general(
            query[:, head, :QK_NOPE],
            keys_nope[:, head],
            (((1,), (1,)), ((), ())),
            preferred_element_type=jnp.float32,
        )
        scores = scores + lax.dot_general(
            query[:, head, QK_NOPE:],
            keys_rope,
            (((1,), (1,)), ((), ())),
            preferred_element_type=jnp.float32,
        )
        scores = scores * score_scale
        if bias_rows is not None:
            scores = scores + bias_rows[head]
        maximum = jnp.max(scores, axis=-1, keepdims=True)
        weights = jnp.exp(scores - maximum)
        totals.append(jnp.sum(weights, axis=-1, keepdims=True))
        maxima.append(maximum)
        accs.append(
            jnp.dot(weights.astype(jnp.bfloat16), values[:, head], preferred_element_type=jnp.float32)
        )
    return accs, maxima, totals


def on_device(
    latent_in,
    condition,
    context_latent,
    context_rope,
    shift_weight,
    scale_weight,
    gate_weight,
    norm_gain,
    down_query,
    down_latent,
    down_rope,
    query_gain,
    latent_gain,
    up_query,
    up_key,
    up_value,
    context_bias,
    out_weight,
):
    sp_at = lax.axis_index("sp")
    tp_at = lax.axis_index("tp")
    tp_size = lax.axis_size("tp")
    local_rows = latent_in.shape[0]
    head_count = up_key.shape[1] // QK_NOPE
    rank = query_gain.shape[0]
    kv_rank = latent_gain.shape[0]

    activated = jax.nn.silu(condition.astype(jnp.float32)).astype(jnp.bfloat16)
    partials = jnp.stack(
        [
            jnp.dot(activated, weight_in, preferred_element_type=jnp.float32)
            for weight_in in (shift_weight, scale_weight, gate_weight)
        ]
    )
    summed = partials
    for piece in gather_pieces(partials, "sp"):
        summed = summed + piece
    context_own = jnp.concatenate([context_latent, context_rope], axis=1)
    context_pieces = [context_own] + gather_pieces(context_own, "sp")
    modulation = lax.all_gather(summed, "tp", axis=1, tiled=True)
    shift_vec = modulation[0]
    scale_vec = modulation[1]
    gate_vec = modulation[2]
    residual_in = latent_in.astype(jnp.float32)
    normed = (rms_scaled(residual_in, norm_gain) * (1.0 + scale_vec) + shift_vec).astype(
        jnp.bfloat16
    )
    query_low = rms_scaled(
        jnp.dot(normed, down_query, preferred_element_type=jnp.float32), query_gain
    ).astype(jnp.bfloat16)
    latent_low = rms_scaled(
        jnp.dot(normed, down_latent, preferred_element_type=jnp.float32), latent_gain
    ).astype(jnp.bfloat16)

    def positions_of(tp_index):
        first_row = (sp_at * tp_size + tp_index) * local_rows
        return first_row + jnp.arange(local_rows, dtype=jnp.int32)

    own_cosine, own_sine = rope_tables(positions_of(tp_at), QK_ROPE)
    rope_keys = rope_turn(
        jnp.dot(normed, down_rope, preferred_element_type=jnp.float32), own_cosine, own_sine
    ).astype(jnp.bfloat16)
    packed = jnp.concatenate([latent_low, rope_keys, query_low], axis=1)
    group = jnp.concatenate([packed] + gather_pieces(packed, "tp"), axis=0)
    origins = [tp_at] + [source(tp_at) for source, _, _ in exchange_steps("tp")]
    key_width = kv_rank + QK_ROPE
    group_keys = group[:, :key_width]
    query_group = group[:, key_width:]
    far_pieces = gather_pieces(group_keys, "sp")

    group_positions = jnp.concatenate([positions_of(origin) for origin in origins])
    group_cosine, group_sine = rope_tables(group_positions, QK_ROPE)
    head_weights = up_query.reshape(rank, head_count, QK_NOPE + QK_ROPE)
    query_nope = jnp.dot(
        query_group,
        head_weights[:, :, :QK_NOPE].reshape(rank, head_count * QK_NOPE),
        preferred_element_type=jnp.float32,
    )
    rope_weights = head_weights[:, :, QK_NOPE:]
    straight = jnp.dot(
        query_group, rope_weights.reshape(rank, -1), preferred_element_type=jnp.float32
    )
    crossed = jnp.dot(
        query_group,
        turn_columns(rope_weights, QK_ROPE).reshape(rank, -1),
        preferred_element_type=jnp.float32,
    )
    group_rows = query_group.shape[0]
    query_rope = straight * jnp.tile(group_cosine, (1, head_count)) + crossed * jnp.tile(
        group_sine, (1, head_count)
    )
    query = jnp.concatenate(
        [
            query_nope.reshape(group_rows, head_count, QK_NOPE),
            query_rope.reshape(group_rows, head_count, QK_ROPE),
        ],
        axis=-1,
    ).astype(jnp.bfloat16)
    near = jnp.concatenate(context_pieces + [group_keys], axis=0)
    context_count = near.shape[0] - group_rows
    near_bias = jnp.concatenate(
        [
            jnp.broadcast_to(context_bias[:, None, None], (head_count, 1, context_count)),
            jnp.zeros((head_count, 1, group_rows), jnp.float32),
        ],
        axis=2,
    )
    parts = [
        attend(query, near[:, :kv_rank], near[:, kv_rank:], up_key, up_value, near_bias)
    ]
    if far_pieces:
        far = jnp.concatenate(far_pieces, axis=0)
        parts.append(
            attend(query, far[:, :kv_rank], far[:, kv_rank:], up_key, up_value, None)
        )
    heads_out = []
    for head in range(head_count):
        maximum = parts[0][1][head]
        for part in parts[1:]:
            maximum = jnp.maximum(maximum, part[1][head])
        acc = 0.0
        total = 0.0
        for part in parts:
            shrink = jnp.exp(part[1][head] - maximum)
            acc = acc + part[0][head] * shrink
            total = total + part[2][head] * shrink
        heads_out.append((acc / total).astype(jnp.bfloat16))
    attended = jnp.concatenate(heads_out, axis=1)
    width = head_count * V_HEAD

    def product(rows_in, origin):
        weight = lax.dynamic_slice_in_dim(out_weight, origin * width, width, axis=0)
        return jnp.dot(rows_in, weight, preferred_element_type=jnp.float32)

    returned = []
    for at, (source, pairs, target) in enumerate(exchange_steps("tp")):
        block = attended[(at + 1) * local_rows : (at + 2) * local_rows]
        back = [(b, a) for a, b in pairs]
        returned.append((lax.ppermute(block, "tp", back), target(tp_at)))
    mixed = product(attended[:local_rows], tp_at)
    for block, origin in returned:
        mixed = mixed + product(block, origin)
    return (residual_in + gate_vec * mixed).astype(jnp.bfloat16)


def solution(mesh):
    in_specs = (
        P(("dp", "sp", "tp"), None),
        P(("dp", "sp")),
        P(("dp", "sp"), None),
        P(("dp", "sp"), None),
        P("sp", "tp"),
        P("sp", "tp"),
        P("sp", "tp"),
        P(),
        P(),
        P(),
        P(),
        P(),
        P(),
        P(None, "tp"),
        P(None, "tp"),
        P(None, "tp"),
        P("tp"),
        P(),
    )
    out_specs = P(("dp", "sp", "tp"), None)
    return jax.shard_map(
        on_device, mesh=mesh, in_specs=in_specs, out_specs=out_specs, check_vma=False
    )
```

```python
import jax
import jax.numpy as jnp
from jax import lax
from jax.sharding import PartitionSpec as P

QK_NOPE = 128
QK_ROPE = 64
V_HEAD = 128
GRID_W = 64


epsilon = 1e-06
rope_base = 10000.0
block_limit = 2048


def rms_scaled(values, gain_vec):
    mean_sq = jnp.mean(values * values, axis=-1, keepdims=True)
    return values * lax.rsqrt(mean_sq + epsilon) * gain_vec


def rope_tables(positions, rope_width):
    freq_count = rope_width // 4
    inverse = rope_base ** (-jnp.arange(freq_count, dtype=jnp.float32) / freq_count)
    grid_row = (positions // GRID_W).astype(jnp.float32)
    grid_col = (positions % GRID_W).astype(jnp.float32)
    row_angle = grid_row[:, None] * inverse
    col_angle = grid_col[:, None] * inverse
    angles = jnp.concatenate([row_angle, row_angle, col_angle, col_angle], axis=-1)
    return (jnp.cos(angles), jnp.sin(angles))


def rope_turn(values, cosine_table, sine_table):
    part_one, part_two, part_three, part_four = jnp.split(values, 4, axis=-1)
    turned = jnp.concatenate([-part_two, part_one, -part_four, part_three], axis=-1)
    return values * cosine_table + turned * sine_table


def exchange_steps(axis):
    size = lax.axis_size(axis)
    steps = list(range(1, size))
    if size & (size - 1):
        return [
            (lambda at, s=s: (at + size - s) % size, [(i, (i + s) % size) for i in range(size)],
             lambda at, s=s: (at + s) % size)
            for s in steps
        ]
    return [(lambda at, s=s: at ^ s, [(i, i ^ s) for i in range(size)], lambda at, s=s: at ^ s) for s in steps]


def in_order(pieces, axis, join):
    size = lax.axis_size(axis)
    at = lax.axis_index(axis)
    stacked = jnp.stack(pieces)
    slots = [(at ^ j) if not size & (size - 1) else (at + size - j) % size for j in range(size)]
    return jnp.concatenate(
        [lax.dynamic_index_in_dim(stacked, slot, 0, keepdims=False) for slot in slots], axis=join
    )


def gather_pieces(piece, axis):
    return [lax.ppermute(piece, axis, pairs) for _, pairs, _ in exchange_steps(axis)]


def attend(query, keys_latent, keys_rope, up_key, up_value, bias_rows):
    head_count = len(query)
    key_count = keys_latent.shape[0]
    score_scale = (QK_NOPE + QK_ROPE) ** (-0.5)
    keys_nope = (
        jnp.dot(keys_latent, up_key, preferred_element_type=jnp.float32)
        .astype(jnp.bfloat16)
        .reshape(key_count, head_count, QK_NOPE)
    )
    values = (
        jnp.dot(keys_latent, up_value, preferred_element_type=jnp.float32)
        .astype(jnp.bfloat16)
        .reshape(key_count, head_count, V_HEAD)
    )
    accs, maxima, totals = [], [], []
    for head in range(head_count):
        scores = lax.dot_general(
            query[head][0],
            keys_nope[:, head],
            (((1,), (1,)), ((), ())),
            preferred_element_type=jnp.float32,
        )
        scores = scores + lax.dot_general(
            query[head][1],
            keys_rope,
            (((1,), (1,)), ((), ())),
            preferred_element_type=jnp.float32,
        )
        scores = scores * score_scale
        if bias_rows is not None:
            scores = scores + bias_rows[head]
        maximum = jnp.max(scores, axis=-1, keepdims=True)
        weights = jnp.exp(scores - maximum)
        totals.append(jnp.sum(weights, axis=-1, keepdims=True))
        maxima.append(maximum)
        accs.append(
            jnp.dot(weights.astype(jnp.bfloat16), values[:, head], preferred_element_type=jnp.float32)
        )
    return accs, maxima, totals


def on_device(
    latent_in,
    condition,
    context_latent,
    context_rope,
    shift_weight,
    scale_weight,
    gate_weight,
    norm_gain,
    down_query,
    down_latent,
    down_rope,
    query_gain,
    latent_gain,
    up_query,
    up_key,
    up_value,
    context_bias,
    out_weight,
):
    sp_at = lax.axis_index("sp")
    tp_at = lax.axis_index("tp")
    tp_size = lax.axis_size("tp")
    local_rows = latent_in.shape[0]
    head_count = up_key.shape[1] // QK_NOPE
    kv_rank = latent_gain.shape[0]

    activated = jax.nn.silu(condition.astype(jnp.float32)).astype(jnp.bfloat16)
    partials = jnp.stack(
        [
            jnp.dot(activated, weight_in, preferred_element_type=jnp.float32)
            for weight_in in (shift_weight, scale_weight, gate_weight)
        ]
    )
    summed = partials
    for piece in gather_pieces(partials, "sp"):
        summed = summed + piece
    modulation = in_order([summed] + gather_pieces(summed, "tp"), "tp", 1)
    context_own = jnp.concatenate([context_latent, context_rope], axis=1)
    context_own, _ = lax.optimization_barrier((context_own, summed))
    context_pieces = [context_own] + gather_pieces(context_own, "sp")
    shift_vec = modulation[0]
    scale_vec = modulation[1]
    gate_vec = modulation[2]
    residual_in = latent_in.astype(jnp.float32)
    normed = (rms_scaled(residual_in, norm_gain) * (1.0 + scale_vec) + shift_vec).astype(
        jnp.bfloat16
    )
    latent_low = rms_scaled(
        jnp.dot(normed, down_latent, preferred_element_type=jnp.float32), latent_gain
    ).astype(jnp.bfloat16)

    def positions_of(tp_index):
        first_row = (sp_at * tp_size + tp_index) * local_rows
        return first_row + jnp.arange(local_rows, dtype=jnp.int32)

    own_cosine, own_sine = rope_tables(positions_of(tp_at), QK_ROPE)
    rope_keys = rope_turn(
        jnp.dot(normed, down_rope, preferred_element_type=jnp.float32), own_cosine, own_sine
    ).astype(jnp.bfloat16)
    own_keys = jnp.concatenate([latent_low, rope_keys], axis=1)
    column_keys = jnp.concatenate([own_keys] + gather_pieces(own_keys, "sp"), axis=0)
    normed_query, context_pieces, _ = lax.optimization_barrier((normed, context_pieces, own_keys))
    query_low = rms_scaled(
        jnp.dot(normed_query, down_query, preferred_element_type=jnp.float32), query_gain
    ).astype(jnp.bfloat16)
    query_group = jnp.concatenate([query_low] + gather_pieces(query_low, "tp"), axis=0)
    far_pieces = gather_pieces(column_keys, "tp")
    origins = [tp_at] + [source(tp_at) for source, _, _ in exchange_steps("tp")]

    group_positions = jnp.concatenate([positions_of(origin) for origin in origins])
    group_cosine, group_sine = rope_tables(group_positions, QK_ROPE)
    group_rows = query_group.shape[0]
    raw = jnp.dot(query_group, up_query, preferred_element_type=jnp.float32)
    query = []
    for head in range(head_count):
        first = head * (QK_NOPE + QK_ROPE)
        query.append(
            (
                raw[:, first : first + QK_NOPE].astype(jnp.bfloat16),
                rope_turn(
                    raw[:, first + QK_NOPE : first + QK_NOPE + QK_ROPE], group_cosine, group_sine
                ).astype(jnp.bfloat16),
            )
        )
    near = jnp.concatenate(context_pieces + [column_keys], axis=0)
    near_rows = column_keys.shape[0]
    context_count = near.shape[0] - near_rows
    near_bias = jnp.concatenate(
        [
            jnp.broadcast_to(context_bias[:, None, None], (head_count, 1, context_count)),
            jnp.zeros((head_count, 1, near_rows), jnp.float32),
        ],
        axis=2,
    )
    parts = [
        attend(query, near[:, :kv_rank], near[:, kv_rank:], up_key, up_value, near_bias)
    ]
    if far_pieces:
        far = jnp.concatenate(far_pieces, axis=0)
        parts.append(
            attend(query, far[:, :kv_rank], far[:, kv_rank:], up_key, up_value, None)
        )
    heads_out = []
    for head in range(head_count):
        maximum = parts[0][1][head]
        for part in parts[1:]:
            maximum = jnp.maximum(maximum, part[1][head])
        acc = 0.0
        total = 0.0
        for part in parts:
            shrink = jnp.exp(part[1][head] - maximum)
            acc = acc + part[0][head] * shrink
            total = total + part[2][head] * shrink
        heads_out.append((acc / total).astype(jnp.bfloat16))
    attended = jnp.concatenate(heads_out, axis=1)
    width = head_count * V_HEAD

    def product(rows_in, origin):
        weight = lax.dynamic_slice_in_dim(out_weight, origin * width, width, axis=0)
        return jnp.dot(rows_in, weight, preferred_element_type=jnp.float32)

    returned = []
    for at, (source, pairs, target) in enumerate(exchange_steps("tp")):
        block = attended[(at + 1) * local_rows : (at + 2) * local_rows]
        back = [(b, a) for a, b in pairs]
        returned.append((lax.ppermute(block, "tp", back), target(tp_at)))
    mixed = product(attended[:local_rows], tp_at)
    for block, origin in returned:
        mixed = mixed + product(block, origin)
    return (residual_in + gate_vec * mixed).astype(jnp.bfloat16)


def solution(mesh):
    in_specs = (
        P(("dp", "sp", "tp"), None),
        P(("dp", "sp")),
        P(("dp", "sp"), None),
        P(("dp", "sp"), None),
        P("sp", "tp"),
        P("sp", "tp"),
        P("sp", "tp"),
        P(),
        P(),
        P(),
        P(),
        P(),
        P(),
        P(None, "tp"),
        P(None, "tp"),
        P(None, "tp"),
        P("tp"),
        P(),
    )
    out_specs = P(("dp", "sp", "tp"), None)
    return jax.shard_map(
        on_device, mesh=mesh, in_specs=in_specs, out_specs=out_specs, check_vma=False
    )
```

```python
import jax
import jax.numpy as jnp
from jax import lax
from jax.experimental import pallas as pl
from jax.experimental.pallas import tpu as pltpu
from jax.sharding import PartitionSpec as P

QK_NOPE = 128
QK_ROPE = 64
V_HEAD = 128
GRID_W = 64


epsilon = 1e-06
rope_base = 10000.0
block_limit = 2048


def rms_scaled(values, gain_vec):
    mean_sq = jnp.mean(values * values, axis=-1, keepdims=True)
    return values * lax.rsqrt(mean_sq + epsilon) * gain_vec


def rope_tables(positions, rope_width):
    freq_count = rope_width // 4
    inverse = rope_base ** (-jnp.arange(freq_count, dtype=jnp.float32) / freq_count)
    grid_row = (positions // GRID_W).astype(jnp.float32)
    grid_col = (positions % GRID_W).astype(jnp.float32)
    row_angle = grid_row[:, None] * inverse
    col_angle = grid_col[:, None] * inverse
    angles = jnp.concatenate([row_angle, row_angle, col_angle, col_angle], axis=-1)
    return (jnp.cos(angles), jnp.sin(angles))


def rope_turn(values, cosine_table, sine_table):
    part_one, part_two, part_three, part_four = jnp.split(values, 4, axis=-1)
    turned = jnp.concatenate([-part_two, part_one, -part_four, part_three], axis=-1)
    return values * cosine_table + turned * sine_table


def exchange_steps(axis):
    size = lax.axis_size(axis)
    steps = list(range(1, size))
    if size & (size - 1):
        return [
            (lambda at, s=s: (at + size - s) % size, [(i, (i + s) % size) for i in range(size)],
             lambda at, s=s: (at + s) % size)
            for s in steps
        ]
    return [(lambda at, s=s: at ^ s, [(i, i ^ s) for i in range(size)], lambda at, s=s: at ^ s) for s in steps]


def modulation_kernel(condition_ref, shift_ref, scale_ref, gate_ref, out_ref):
    values = condition_ref[...].astype(jnp.float32)
    activated = values / (1.0 + jnp.exp(-values))
    rows = jnp.broadcast_to(activated, (16, values.shape[1])).astype(jnp.bfloat16)
    for row, weight_ref in enumerate((shift_ref, scale_ref, gate_ref)):
        product = jnp.dot(rows, weight_ref[...], preferred_element_type=jnp.float32)
        out_ref[row : row + 1, :] = product[0:1]


def modulation_partials(condition, *weights):
    vmem = pl.BlockSpec(memory_space=pltpu.VMEM)
    return pl.pallas_call(
        modulation_kernel,
        out_shape=jax.ShapeDtypeStruct((len(weights), weights[0].shape[1]), jnp.float32),
        in_specs=[vmem] * (1 + len(weights)),
        out_specs=vmem,
        name="modulation",
    )(condition[None, :], *weights)


def in_order(pieces, axis, join):
    size = lax.axis_size(axis)
    at = lax.axis_index(axis)
    stacked = jnp.stack(pieces)
    slots = [(at ^ j) if not size & (size - 1) else (at + size - j) % size for j in range(size)]
    return jnp.concatenate(
        [lax.dynamic_index_in_dim(stacked, slot, 0, keepdims=False) for slot in slots], axis=join
    )


def gather_pieces(piece, axis):
    return [lax.ppermute(piece, axis, pairs) for _, pairs, _ in exchange_steps(axis)]


def attend(query, keys_latent, keys_rope, up_key, up_value, bias_rows):
    head_count = len(query)
    key_count = keys_latent.shape[0]
    score_scale = (QK_NOPE + QK_ROPE) ** (-0.5)
    keys_nope = (
        jnp.dot(keys_latent, up_key, preferred_element_type=jnp.float32)
        .astype(jnp.bfloat16)
        .reshape(key_count, head_count, QK_NOPE)
    )
    values = (
        jnp.dot(keys_latent, up_value, preferred_element_type=jnp.float32)
        .astype(jnp.bfloat16)
        .reshape(key_count, head_count, V_HEAD)
    )
    accs, maxima, totals = [], [], []
    for head in range(head_count):
        scores = lax.dot_general(
            query[head][0],
            keys_nope[:, head],
            (((1,), (1,)), ((), ())),
            preferred_element_type=jnp.float32,
        )
        scores = scores + lax.dot_general(
            query[head][1],
            keys_rope,
            (((1,), (1,)), ((), ())),
            preferred_element_type=jnp.float32,
        )
        scores = scores * score_scale
        if bias_rows is not None:
            scores = scores + bias_rows[head]
        maximum = jnp.max(scores, axis=-1, keepdims=True)
        weights = jnp.exp(scores - maximum)
        totals.append(jnp.sum(weights, axis=-1, keepdims=True))
        maxima.append(maximum)
        accs.append(
            jnp.dot(weights.astype(jnp.bfloat16), values[:, head], preferred_element_type=jnp.float32)
        )
    return accs, maxima, totals


def on_device(
    latent_in,
    condition,
    context_latent,
    context_rope,
    shift_weight,
    scale_weight,
    gate_weight,
    norm_gain,
    down_query,
    down_latent,
    down_rope,
    query_gain,
    latent_gain,
    up_query,
    up_key,
    up_value,
    context_bias,
    out_weight,
):
    sp_at = lax.axis_index("sp")
    tp_at = lax.axis_index("tp")
    tp_size = lax.axis_size("tp")
    local_rows = latent_in.shape[0]
    head_count = up_key.shape[1] // QK_NOPE
    kv_rank = latent_gain.shape[0]

    partials = modulation_partials(condition, shift_weight, scale_weight, gate_weight)
    summed = partials
    for piece in gather_pieces(partials, "sp"):
        summed = summed + piece
    modulation = in_order([summed] + gather_pieces(summed, "tp"), "tp", 1)
    shift_vec = modulation[0]
    scale_vec = modulation[1]
    gate_vec = modulation[2]
    residual_in = latent_in.astype(jnp.float32)
    normed = (rms_scaled(residual_in, norm_gain) * (1.0 + scale_vec) + shift_vec).astype(
        jnp.bfloat16
    )
    latent_low = rms_scaled(
        jnp.dot(normed, down_latent, preferred_element_type=jnp.float32), latent_gain
    ).astype(jnp.bfloat16)

    def positions_of(tp_index):
        first_row = (sp_at * tp_size + tp_index) * local_rows
        return first_row + jnp.arange(local_rows, dtype=jnp.int32)

    own_cosine, own_sine = rope_tables(positions_of(tp_at), QK_ROPE)
    rope_keys = rope_turn(
        jnp.dot(normed, down_rope, preferred_element_type=jnp.float32), own_cosine, own_sine
    ).astype(jnp.bfloat16)
    own_keys = jnp.concatenate([latent_low, rope_keys], axis=1)
    context_own = jnp.concatenate([context_latent, context_rope], axis=1)
    sent_keys = jnp.concatenate([own_keys, context_own], axis=0)
    key_pieces = [sent_keys] + gather_pieces(sent_keys, "sp")
    near = jnp.concatenate(key_pieces, axis=0)
    normed_query, _ = lax.optimization_barrier((normed, sent_keys))
    query_low = rms_scaled(
        jnp.dot(normed_query, down_query, preferred_element_type=jnp.float32), query_gain
    ).astype(jnp.bfloat16)
    query_group = jnp.concatenate([query_low] + gather_pieces(query_low, "tp"), axis=0)
    column_keys = jnp.concatenate([piece[:local_rows] for piece in key_pieces], axis=0)
    column_keys, _ = lax.optimization_barrier((column_keys, query_low))
    far_pieces = gather_pieces(column_keys, "tp")
    origins = [tp_at] + [source(tp_at) for source, _, _ in exchange_steps("tp")]

    group_positions = jnp.concatenate([positions_of(origin) for origin in origins])
    group_cosine, group_sine = rope_tables(group_positions, QK_ROPE)
    group_rows = query_group.shape[0]
    raw = jnp.dot(query_group, up_query, preferred_element_type=jnp.float32)
    query = []
    for head in range(head_count):
        first = head * (QK_NOPE + QK_ROPE)
        query.append(
            (
                raw[:, first : first + QK_NOPE].astype(jnp.bfloat16),
                rope_turn(
                    raw[:, first + QK_NOPE : first + QK_NOPE + QK_ROPE], group_cosine, group_sine
                ).astype(jnp.bfloat16),
            )
        )
    bias_piece = jnp.concatenate(
        [
            jnp.zeros((head_count, 1, local_rows), jnp.float32),
            jnp.broadcast_to(
                context_bias[:, None, None], (head_count, 1, context_latent.shape[0])
            ),
        ],
        axis=2,
    )
    near_bias = jnp.concatenate([bias_piece] * len(key_pieces), axis=2)
    parts = [
        attend(query, near[:, :kv_rank], near[:, kv_rank:], up_key, up_value, near_bias)
    ]
    if far_pieces:
        far = jnp.concatenate(far_pieces, axis=0)
        parts.append(
            attend(query, far[:, :kv_rank], far[:, kv_rank:], up_key, up_value, None)
        )
    heads_out = []
    for head in range(head_count):
        maximum = parts[0][1][head]
        for part in parts[1:]:
            maximum = jnp.maximum(maximum, part[1][head])
        acc = 0.0
        total = 0.0
        for part in parts:
            shrink = jnp.exp(part[1][head] - maximum)
            acc = acc + part[0][head] * shrink
            total = total + part[2][head] * shrink
        heads_out.append((acc / total).astype(jnp.bfloat16))
    attended = jnp.concatenate(heads_out, axis=1)
    width = head_count * V_HEAD

    def product(rows_in, origin):
        weight = lax.dynamic_slice_in_dim(out_weight, origin * width, width, axis=0)
        return jnp.dot(rows_in, weight, preferred_element_type=jnp.float32)

    returned = []
    for at, (source, pairs, target) in enumerate(exchange_steps("tp")):
        block = attended[(at + 1) * local_rows : (at + 2) * local_rows]
        back = [(b, a) for a, b in pairs]
        returned.append((lax.ppermute(block, "tp", back), target(tp_at)))
    mixed = product(attended[:local_rows], tp_at)
    for block, origin in returned:
        mixed = mixed + product(block, origin)
    return (residual_in + gate_vec * mixed).astype(jnp.bfloat16)


def solution(mesh):
    in_specs = (
        P(("dp", "sp", "tp"), None),
        P(("dp", "sp")),
        P(("dp", "sp"), None),
        P(("dp", "sp"), None),
        P("sp", "tp"),
        P("sp", "tp"),
        P("sp", "tp"),
        P(),
        P(),
        P(),
        P(),
        P(),
        P(),
        P(None, "tp"),
        P(None, "tp"),
        P(None, "tp"),
        P("tp"),
        P(),
    )
    out_specs = P(("dp", "sp", "tp"), None)
    return jax.shard_map(
        on_device, mesh=mesh, in_specs=in_specs, out_specs=out_specs, check_vma=False
    )
```

```python
import jax
import jax.numpy as jnp
from jax import lax
from jax.experimental import pallas as pl
from jax.experimental.pallas import tpu as pltpu
from jax.sharding import PartitionSpec as P

QK_NOPE = 128
QK_ROPE = 64
V_HEAD = 128
GRID_W = 64


epsilon = 1e-06
rope_base = 10000.0
block_limit = 2048


def rms_scaled(values, gain_vec):
    mean_sq = jnp.mean(values * values, axis=-1, keepdims=True)
    return values * lax.rsqrt(mean_sq + epsilon) * gain_vec


def rope_tables(positions, rope_width):
    freq_count = rope_width // 4
    inverse = rope_base ** (-jnp.arange(freq_count, dtype=jnp.float32) / freq_count)
    grid_row = (positions // GRID_W).astype(jnp.float32)
    grid_col = (positions % GRID_W).astype(jnp.float32)
    row_angle = grid_row[:, None] * inverse
    col_angle = grid_col[:, None] * inverse
    angles = jnp.concatenate([row_angle, row_angle, col_angle, col_angle], axis=-1)
    return (jnp.cos(angles), jnp.sin(angles))


def rope_turn(values, cosine_table, sine_table):
    part_one, part_two, part_three, part_four = jnp.split(values, 4, axis=-1)
    turned = jnp.concatenate([-part_two, part_one, -part_four, part_three], axis=-1)
    return values * cosine_table + turned * sine_table


def exchange_steps(axis):
    size = lax.axis_size(axis)
    steps = list(range(1, size))
    if size & (size - 1):
        return [
            (lambda at, s=s: (at + size - s) % size, [(i, (i + s) % size) for i in range(size)],
             lambda at, s=s: (at + s) % size)
            for s in steps
        ]
    return [(lambda at, s=s: at ^ s, [(i, i ^ s) for i in range(size)], lambda at, s=s: at ^ s) for s in steps]


def modulation_kernel(condition_ref, shift_ref, scale_ref, gate_ref, out_ref):
    values = condition_ref[...].astype(jnp.float32)
    activated = values / (1.0 + jnp.exp(-values))
    rows = jnp.broadcast_to(activated, (16, values.shape[1])).astype(jnp.bfloat16)
    for row, weight_ref in enumerate((shift_ref, scale_ref, gate_ref)):
        product = jnp.dot(rows, weight_ref[...], preferred_element_type=jnp.float32)
        out_ref[row : row + 1, :] = product[0:1]


def modulation_partials(condition, *weights):
    vmem = pl.BlockSpec(memory_space=pltpu.VMEM)
    return pl.pallas_call(
        modulation_kernel,
        out_shape=jax.ShapeDtypeStruct((len(weights), weights[0].shape[1]), jnp.float32),
        in_specs=[vmem] * (1 + len(weights)),
        out_specs=vmem,
        name="modulation",
    )(condition[None, :], *weights)


def in_order(pieces, axis, join):
    size = lax.axis_size(axis)
    at = lax.axis_index(axis)
    stacked = jnp.stack(pieces)
    slots = [(at ^ j) if not size & (size - 1) else (at + size - j) % size for j in range(size)]
    return jnp.concatenate(
        [lax.dynamic_index_in_dim(stacked, slot, 0, keepdims=False) for slot in slots], axis=join
    )


def gather_pieces(piece, axis):
    return [lax.ppermute(piece, axis, pairs) for _, pairs, _ in exchange_steps(axis)]


def attend(query, keys_latent, keys_rope, up_key, up_value, bias_rows):
    head_count = len(query)
    key_count = keys_latent.shape[0]
    score_scale = (QK_NOPE + QK_ROPE) ** (-0.5)
    keys_nope = (
        jnp.dot(keys_latent, up_key, preferred_element_type=jnp.float32)
        .astype(jnp.bfloat16)
        .reshape(key_count, head_count, QK_NOPE)
    )
    values = (
        jnp.dot(keys_latent, up_value, preferred_element_type=jnp.float32)
        .astype(jnp.bfloat16)
        .reshape(key_count, head_count, V_HEAD)
    )
    accs, maxima, totals = [], [], []
    for head in range(head_count):
        scores = lax.dot_general(
            query[head][0],
            keys_nope[:, head],
            (((1,), (1,)), ((), ())),
            preferred_element_type=jnp.float32,
        )
        scores = scores + lax.dot_general(
            query[head][1],
            keys_rope,
            (((1,), (1,)), ((), ())),
            preferred_element_type=jnp.float32,
        )
        scores = scores * score_scale
        if bias_rows is not None:
            scores = scores + bias_rows[head]
        maximum = jnp.max(scores, axis=-1, keepdims=True)
        weights = jnp.exp(scores - maximum)
        totals.append(jnp.sum(weights, axis=-1, keepdims=True))
        maxima.append(maximum)
        accs.append(
            jnp.dot(weights.astype(jnp.bfloat16), values[:, head], preferred_element_type=jnp.float32)
        )
    return accs, maxima, totals


def on_device(
    latent_in,
    condition,
    context_latent,
    context_rope,
    shift_weight,
    scale_weight,
    gate_weight,
    norm_gain,
    down_query,
    down_latent,
    down_rope,
    query_gain,
    latent_gain,
    up_query,
    up_key,
    up_value,
    context_bias,
    out_weight,
):
    sp_at = lax.axis_index("sp")
    tp_at = lax.axis_index("tp")
    tp_size = lax.axis_size("tp")
    local_rows = latent_in.shape[0]
    head_count = up_key.shape[1] // QK_NOPE
    kv_rank = latent_gain.shape[0]

    partials = modulation_partials(condition, shift_weight, scale_weight, gate_weight)
    summed = partials
    for piece in gather_pieces(partials, "sp"):
        summed = summed + piece
    modulation = in_order([summed] + gather_pieces(summed, "tp"), "tp", 1)
    shift_vec = modulation[0]
    scale_vec = modulation[1]
    gate_vec = modulation[2]
    residual_in = latent_in.astype(jnp.float32)
    normed = (rms_scaled(residual_in, norm_gain) * (1.0 + scale_vec) + shift_vec).astype(
        jnp.bfloat16
    )
    latent_low = rms_scaled(
        jnp.dot(normed, down_latent, preferred_element_type=jnp.float32), latent_gain
    ).astype(jnp.bfloat16)

    def positions_of(tp_index):
        first_row = (sp_at * tp_size + tp_index) * local_rows
        return first_row + jnp.arange(local_rows, dtype=jnp.int32)

    own_cosine, own_sine = rope_tables(positions_of(tp_at), QK_ROPE)
    rope_keys = rope_turn(
        jnp.dot(normed, down_rope, preferred_element_type=jnp.float32), own_cosine, own_sine
    ).astype(jnp.bfloat16)
    own_keys = jnp.concatenate([latent_low, rope_keys], axis=1)
    context_own = jnp.concatenate([context_latent, context_rope], axis=1)
    sent_keys = jnp.concatenate([own_keys, context_own], axis=0)
    key_pieces = [sent_keys] + gather_pieces(sent_keys, "sp")
    near = jnp.concatenate(key_pieces, axis=0)
    normed_query, _ = lax.optimization_barrier((normed, sent_keys))
    query_low = rms_scaled(
        jnp.dot(normed_query, down_query, preferred_element_type=jnp.float32), query_gain
    ).astype(jnp.bfloat16)
    query_pieces = [query_low] + gather_pieces(query_low, "tp")
    column_keys = jnp.concatenate([piece[:local_rows] for piece in key_pieces], axis=0)
    column_keys, _ = lax.optimization_barrier((column_keys, query_low))
    far_pieces = gather_pieces(column_keys, "tp")
    query_pieces, _ = lax.optimization_barrier((query_pieces, column_keys))
    query_group = jnp.concatenate(query_pieces, axis=0)
    origins = [tp_at] + [source(tp_at) for source, _, _ in exchange_steps("tp")]

    group_positions = jnp.concatenate([positions_of(origin) for origin in origins])
    group_cosine, group_sine = rope_tables(group_positions, QK_ROPE)
    group_rows = query_group.shape[0]
    raw = jnp.dot(query_group, up_query, preferred_element_type=jnp.float32)
    query = []
    for head in range(head_count):
        first = head * (QK_NOPE + QK_ROPE)
        query.append(
            (
                raw[:, first : first + QK_NOPE].astype(jnp.bfloat16),
                rope_turn(
                    raw[:, first + QK_NOPE : first + QK_NOPE + QK_ROPE], group_cosine, group_sine
                ).astype(jnp.bfloat16),
            )
        )
    bias_piece = jnp.concatenate(
        [
            jnp.zeros((head_count, 1, local_rows), jnp.float32),
            jnp.broadcast_to(
                context_bias[:, None, None], (head_count, 1, context_latent.shape[0])
            ),
        ],
        axis=2,
    )
    near_bias = jnp.concatenate([bias_piece] * len(key_pieces), axis=2)
    parts = [
        attend(query, near[:, :kv_rank], near[:, kv_rank:], up_key, up_value, near_bias)
    ]
    for arrived in (far_pieces[:1], far_pieces[1:]):
        if not arrived:
            continue
        far = jnp.concatenate(arrived, axis=0)
        parts.append(
            attend(query, far[:, :kv_rank], far[:, kv_rank:], up_key, up_value, None)
        )
    heads_out = []
    for head in range(head_count):
        maximum = parts[0][1][head]
        for part in parts[1:]:
            maximum = jnp.maximum(maximum, part[1][head])
        acc = 0.0
        total = 0.0
        for part in parts:
            shrink = jnp.exp(part[1][head] - maximum)
            acc = acc + part[0][head] * shrink
            total = total + part[2][head] * shrink
        heads_out.append((acc / total).astype(jnp.bfloat16))
    attended = jnp.concatenate(heads_out, axis=1)
    width = head_count * V_HEAD

    def product(rows_in, origin):
        weight = lax.dynamic_slice_in_dim(out_weight, origin * width, width, axis=0)
        return jnp.dot(rows_in, weight, preferred_element_type=jnp.float32)

    returned = []
    for at, (source, pairs, target) in enumerate(exchange_steps("tp")):
        block = attended[(at + 1) * local_rows : (at + 2) * local_rows]
        back = [(b, a) for a, b in pairs]
        returned.append((lax.ppermute(block, "tp", back), target(tp_at)))
    mixed = product(attended[:local_rows], tp_at)
    for block, origin in returned:
        mixed = mixed + product(block, origin)
    return (residual_in + gate_vec * mixed).astype(jnp.bfloat16)


def solution(mesh):
    in_specs = (
        P(("dp", "sp", "tp"), None),
        P(("dp", "sp")),
        P(("dp", "sp"), None),
        P(("dp", "sp"), None),
        P("sp", "tp"),
        P("sp", "tp"),
        P("sp", "tp"),
        P(),
        P(),
        P(),
        P(),
        P(),
        P(),
        P(None, "tp"),
        P(None, "tp"),
        P(None, "tp"),
        P("tp"),
        P(),
    )
    out_specs = P(("dp", "sp", "tp"), None)
    return jax.shard_map(
        on_device, mesh=mesh, in_specs=in_specs, out_specs=out_specs, check_vma=False
    )
```
